32 devices in a mesh: ep: 8 (over z, core), tp: 4 (over y, x).
Axes of the slice: x: 2, y: 2, z: 4, core: 2. Of those that a mesh axis runs over, the one named last changes fastest.
Arguments:
- queries: bfloat16 [1024, 4096], P('ep', 'tp'), may hold values from -32 to 32
- keys: bfloat16 [1024, 2048], P('ep', 'tp'), may hold values from -32 to 32
- values: bfloat16 [1024, 2048], P('ep', 'tp'), may hold values from -6 to 6
- query_gain: float32 [128], replicated, may hold values from 1 to 6
- key_gain: float32 [128], replicated, may hold values from 1 to 6
- out_weight: bfloat16 [4096, 2048], P('tp'), may hold values from -0.75 to 0.75
- expert_input: bfloat16 [1024, 2048], P('ep'), may hold values from -64 to 64
- norm_gain: float32 [2048], replicated, may hold values from 0.1 to 1.9
- routes: int32 [1024, 2], P('ep'), may hold values from 0 to 7, all different within a row; in each aligned block of 128 rows (0 to 127, 128 to 255, ...) at most 40 rows name the same one
- route_logits: float32 [1024, 2], P('ep'), may hold values from -6 to 6
- gate_weight: bfloat16 [8, 2048, 2816], P('ep', None, 'tp'), may hold values from -0.125 to 0.125
- up_weight: bfloat16 [8, 2048, 2816], P('ep', None, 'tp'), may hold values from -0.125 to 0.125
- down_weight: bfloat16 [8, 2816, 2048], P('ep', 'tp'), may hold values from -0.109375 to 0.109375
Outputs:
- mixed: bfloat16 [1024, 2048], P(('ep', 'tp'))
- expert_out: bfloat16 [1024, 2048], P('ep', 'tp')
The draws below stay inside these ranges and needn't reach their ends.
Inputs may be any that keep to these rules, and one draw needn't show every extreme that they name: `routes`: A token's 2 experts differ. Among the 128 tokens of one index of ep (aligned blocks), no expert is named by more than 40 tokens, a bound that some block reaches.
All inputs are finite; a program needn't handle non-finite values.
Results may differ from the reference program's by a relative error of at most 0.015.
The reference program's roundings to bfloat16 on the way count: a program that leaves them out, or rounds other values in their place, can miss the bound.
Values may be sent and summed in bfloat16 or wider, within the bound.
No kernel may reach another device: no remote copies, remote signals or barrier semaphores. Data moves between devices by JAX's collectives and lax.ppermute only.
A program may use at most 64 MiB of HBM per device.

```python
import math
import jax
import jax.numpy as jnp
import numpy as np
from jax import lax

D = 2048
HEADS = 32
KV_HEADS = 16
HEAD_DIM = 128
GROUP = 2
GRID_W = 64
FF_E = 2816
TOP_K = 2
TOK_B = 128
TOKENS_A = 1024
TOKENS_B = 1024
EXPERTS = 8
CAP = 40
N_EP = 8
N_TP = 4


def query_key_pair(key):
    base = jax.random.fold_in(key, 5)
    key_q, key_k, scale_q, scale_k = jax.random.split(base, 4)
    q_cols = HEADS * HEAD_DIM
    k_cols = KV_HEADS * HEAD_DIM
    q_raw = jnp.clip(jax.random.normal(key_q, (TOKENS_A, q_cols), jnp.float32), -6.0, 6.0)
    k_raw = jnp.clip(jax.random.normal(key_k, (TOKENS_A, k_cols), jnp.float32), -6.0, 6.0)
    q_scale = jnp.exp(jax.random.uniform(scale_q, (q_cols,), jnp.float32, jnp.log(0.5), jnp.log(5.0)))
    k_scale = jnp.exp(jax.random.uniform(scale_k, (k_cols,), jnp.float32, jnp.log(0.5), jnp.log(5.0)))
    q_data = q_raw * q_scale
    k_data = k_raw * k_scale
    return (jnp.clip(q_data, -32.0, 32.0), jnp.clip(k_data, -32.0, 32.0))


def draw_queries(key, part):
    return query_key_pair(key)[0].astype(jnp.bfloat16)


def draw_keys(key, part):
    return query_key_pair(key)[1].astype(jnp.bfloat16)


def draw_query_gain(key, part):
    own = jax.random.fold_in(key, 11)
    return jax.random.uniform(own, (HEAD_DIM,), jnp.float32, 1.0, 1.8)


def draw_key_gain(key, part):
    own = jax.random.fold_in(key, 13)
    return jax.random.uniform(own, (HEAD_DIM,), jnp.float32, 1.0, 1.8)


def draw_expert_input(key, part):
    own = jax.random.fold_in(key, 17)
    key_x, key_row, key_col = jax.random.split(own, 3)
    col_scale = jnp.exp(jax.random.uniform(key_col, (D,), jnp.float32, jnp.log(0.3), jnp.log(3.0)))
    raw = jnp.clip(jax.random.normal(key_x, (TOKENS_B, D), jnp.float32), -6.0, 6.0)
    row_scale = jnp.exp(jax.random.uniform(key_row, (TOKENS_B, 1), jnp.float32, jnp.log(0.3), jnp.log(3.0)))
    return jnp.clip(raw * row_scale * col_scale, -64.0, 64.0).astype(jnp.bfloat16)


def steps_of(stream_key, shape, cuts, least, largest):
    def one(axis_at, blocks):
        draws = jax.random.uniform(jax.random.fold_in(jax.random.fold_in(stream_key, 6), axis_at), (blocks,), jnp.float32, least / len(cuts), largest / len(cuts))
        return jnp.repeat(jnp.exp(draws), shape[axis_at] // blocks).reshape((-1,) + (1,) * (len(shape) - axis_at - 1))

    level = one(*cuts[0])
    for cut in cuts[1:]:
        level = level * one(*cut)
    return level


def deal_out(own_key, own, number, rows, number_of, top, limit, skew):
    sequence = jax.random.permutation(own_key, number_of)
    crowded, ordinary = load_shares(number_of, rows * top, limit, skew, True), load_shares(number_of, rows * top, limit, skew, False)
    places = jnp.arange(number_of)

    def named(lengths, turn):
        used = int((lengths > 0).sum())
        fixed = max(1, used // 4)
        moved = fixed + (places - fixed + turn * (used - fixed)) % max(1, number_of - fixed)
        return jnp.zeros((number_of,), jnp.int32).at[sequence[jnp.where(places < fixed, places, moved)]].set(jnp.asarray(lengths, jnp.int32))

    lengths = jnp.where(number % 4 == 0, named(crowded, number // 4), named(ordinary, number - number // 4 - 1))
    mixed = jax.random.permutation(jax.random.fold_in(own, 3), number_of)
    giver, taker = mixed[0:number_of // 2 * 2:2], mixed[1:number_of // 2 * 2:2]
    room = jnp.minimum(lengths[giver] - 1, limit - lengths[taker]) // 2
    room = jnp.where((giver == sequence[0]) | (taker == sequence[0]) | (lengths[taker] == 0), 0, jnp.maximum(room, 0))
    moved = jax.random.randint(jax.random.fold_in(own, 4), (number_of // 2,), 0, 1 << 20) % (room + 1)
    lengths = lengths.at[giver].add(-moved).at[taker].add(moved)
    labels = jnp.searchsorted(jnp.cumsum(lengths), jnp.arange(rows * top), side="right").astype(jnp.int32)
    table = labels.reshape(top, rows).T
    table = table[jax.random.permutation(jax.random.fold_in(own, 1), rows)]
    turn = jax.random.randint(jax.random.fold_in(own, 2), (rows, 1), 0, top)
    return jnp.take_along_axis(table, (jnp.arange(top)[None, :] + turn) % top, axis=1)


def load_shares(number_of, total, limit, skew, full):
    portions = [(1 << 20) // math.isqrt(rank ** skew) + 1 for rank in range(1, number_of + 1)]
    largest = limit if full else min(limit, max(-(-total // number_of), total * portions[0] // sum(portions)))
    least = 1 if total - largest >= number_of - 1 else 0
    counts, surplus = [largest] + [least] * (number_of - 1), total - largest - least * (number_of - 1)
    while surplus > 0:
        movable = [i for i in range(1, number_of) if counts[i] < largest] or [i for i in range(1, number_of) if counts[i] < limit]
        pool, remaining = sum([portions[i] for i in movable]), surplus
        for i in movable:
            extra = min(limit - counts[i], max(1, remaining * portions[i] // pool), surplus)
            counts[i] = counts[i] + extra
            surplus = surplus - extra
    return np.array(counts)


def centred(stream_key, extent, deviation, limit, pieces=(), kind=jnp.bfloat16):
    result = deviation * jax.random.normal(stream_key, extent, jnp.float32)
    if pieces:
        result = result * steps_of(stream_key, extent, pieces, -0.22, 0.18)
    return jnp.clip(result, -limit, limit).astype(kind)


def setup_inputs(seed: int = 0) -> dict:
    seeds = jax.random.split(jax.random.key(seed), 14)
    queries = draw_queries(jax.random.fold_in(seeds[13], 71), 0)
    keys = draw_keys(jax.random.fold_in(seeds[13], 71), 0)
    values = centred(seeds[2], (TOKENS_A, KV_HEADS * HEAD_DIM), 1.0, 6.0, ((0, 8), (1, 4)))
    query_gain = draw_query_gain(jax.random.fold_in(seeds[13], 71), 0)
    key_gain = draw_key_gain(jax.random.fold_in(seeds[13], 71), 0)
    out_weight = centred(seeds[5], (HEADS * HEAD_DIM, D), (HEADS * HEAD_DIM // 64) ** -0.5, 0.75, ((0, 4),))
    expert_input = draw_expert_input(jax.random.fold_in(seeds[13], 71), 0)
    norm_gain = jnp.clip(1.0 + 0.18 * jax.random.normal(seeds[7], (D,), jnp.float32), 0.1, 1.9)
    routes_keys = jax.random.split(jax.random.fold_in(seeds[8], 1), TOKENS_B // TOK_B)
    routes_turns = jax.random.permutation(jax.random.fold_in(seeds[8], 3), TOKENS_B // TOK_B)
    routes = jax.vmap(lambda own, number: deal_out(jax.random.fold_in(seeds[8], 2), own, number, TOK_B, EXPERTS, TOP_K, CAP, 0))(routes_keys, routes_turns).reshape((TOKENS_B, TOP_K))
    route_logits = centred(seeds[9], (TOKENS_B, TOP_K), 1.5, 6.0, ((0, 8),), jnp.float32)
    gate_weight = centred(seeds[10], (EXPERTS, D, FF_E), D ** -0.5, 0.125, ((0, 8), (2, 4)))
    up_weight = centred(seeds[11], (EXPERTS, D, FF_E), D ** -0.5, 0.125, ((0, 8), (2, 4)))
    down_weight = centred(seeds[12], (EXPERTS, FF_E, D), FF_E ** -0.5, 0.109375, ((0, 8), (1, 4)))
    return dict(queries=queries, keys=keys, values=values, query_gain=query_gain, key_gain=key_gain, out_weight=out_weight, expert_input=expert_input, norm_gain=norm_gain, routes=routes, route_logits=route_logits, gate_weight=gate_weight, up_weight=up_weight, down_weight=down_weight)


def rope_tables(count, head_dim):
    pos = jnp.arange(count, dtype=jnp.int32)
    grid_row = (pos // GRID_W).astype(jnp.float32)
    grid_col = (pos % GRID_W).astype(jnp.float32)
    quarter = head_dim // 4
    inverse = 10000.0 ** (-jnp.arange(quarter, dtype=jnp.float32) / quarter)
    angles = jnp.concatenate([grid_row[:, None] * inverse, grid_col[:, None] * inverse], axis=-1)
    return (jnp.cos(angles), jnp.sin(angles))

def norm_rotate(x, gain, cosine, sine):
    count, number, head_dim = x.shape
    y = x * lax.rsqrt(lax.optimization_barrier(jnp.mean(x * x, axis=-1, keepdims=True)) + 1e-06) * gain
    pairs = y.reshape(count, number, head_dim // 2, 2)
    first, second = (pairs[..., 0], pairs[..., 1])
    cos_b = cosine[:, None, :]
    sin_b = sine[:, None, :]
    turned = jnp.stack([first * cos_b - second * sin_b, first * sin_b + second * cos_b], axis=-1)
    return turned.reshape(count, number, head_dim).astype(jnp.bfloat16)

def round_sum(lefts, rights):

    def add_part(total, pair):
        part = jnp.dot(pair[0], pair[1], preferred_element_type=jnp.float32).astype(jnp.bfloat16)
        part = lax.optimization_barrier(part)
        return (total + part.astype(jnp.float32), None)
    start = jnp.zeros((lefts.shape[1], rights.shape[2]), jnp.float32)
    total, _ = lax.scan(add_part, start, (lefts, rights))
    return total.astype(jnp.bfloat16)

def reference(queries, keys, values, query_gain, key_gain, out_weight, expert_input, norm_gain, routes, route_logits, gate_weight, up_weight, down_weight):
    cosine, sine = rope_tables(TOKENS_A, HEAD_DIM)
    q_rot = norm_rotate(queries.astype(jnp.float32).reshape(TOKENS_A, HEADS, HEAD_DIM), query_gain, cosine, sine)
    k_rot = norm_rotate(keys.astype(jnp.float32).reshape(TOKENS_A, KV_HEADS, HEAD_DIM), key_gain, cosine, sine)
    v_heads = values.reshape(TOKENS_A, KV_HEADS, HEAD_DIM)
    q_all = q_rot.transpose(1, 0, 2)
    k_all = jnp.repeat(k_rot, GROUP, axis=1).transpose(1, 0, 2)
    v_all = jnp.repeat(v_heads, GROUP, axis=1).transpose(1, 0, 2)
    block = math.gcd(TOKENS_A, 1024)
    scale = HEAD_DIM ** (-0.5)

    def one_head(args):
        q_head, k_head, v_head = args

        def one_block(q_block):
            scores = jnp.dot(q_block, k_head.T, preferred_element_type=jnp.float32) * scale
            peak = lax.optimization_barrier(jnp.max(scores, axis=-1, keepdims=True))
            weights = jnp.exp(scores - peak)
            total = lax.optimization_barrier(jnp.sum(weights, axis=-1, keepdims=True))
            summed = jnp.dot(weights.astype(jnp.bfloat16), v_head, preferred_element_type=jnp.float32)
            return (summed / total).astype(jnp.bfloat16)
        return lax.map(one_block, q_head.reshape(TOKENS_A // block, block, HEAD_DIM)).reshape(TOKENS_A, HEAD_DIM)
    attended = lax.map(one_head, (q_all, k_all, v_all)).transpose(1, 0, 2).reshape(TOKENS_A, HEADS * HEAD_DIM)
    width = HEADS * HEAD_DIM // N_TP
    mixed = round_sum(attended.reshape(TOKENS_A, N_TP, width).transpose(1, 0, 2), out_weight.reshape(N_TP, width, D))
    x = expert_input.astype(jnp.float32)
    normed = (x * lax.rsqrt(lax.optimization_barrier(jnp.mean(x * x, axis=-1, keepdims=True)) + 1e-06) * norm_gain).astype(jnp.bfloat16)
    route_weight = jax.nn.sigmoid(route_logits - route_logits[:, ::-1])
    ids = routes.reshape(N_EP, TOK_B * TOP_K)
    onehot = (ids[..., None] == jnp.arange(EXPERTS, dtype=jnp.int32)).astype(jnp.int32)
    before = jnp.cumsum(onehot, axis=1) - onehot
    slot = lax.optimization_barrier(jnp.sum(before * onehot, axis=-1))
    source = jnp.broadcast_to(jnp.arange(N_EP, dtype=jnp.int32)[:, None], ids.shape)
    token = source * TOK_B + jnp.arange(TOK_B * TOP_K, dtype=jnp.int32)[None, :] // TOP_K
    table = jnp.full((EXPERTS, N_EP, CAP), TOKENS_B, jnp.int32).at[ids, source, slot].set(token)
    padded = jnp.concatenate([normed, jnp.zeros((1, D), jnp.bfloat16)], axis=0)
    hidden_block = FF_E // N_TP

    def one_expert(args):
        rows_index, w_gate, w_up, w_down = args
        rows = padded[rows_index.reshape(-1)]
        gate = jnp.dot(rows, w_gate, preferred_element_type=jnp.float32)
        upper = jnp.dot(rows, w_up, preferred_element_type=jnp.float32)
        hidden = (jax.nn.silu(gate) * upper).astype(jnp.bfloat16)
        count = rows.shape[0]
        return round_sum(hidden.reshape(count, N_TP, hidden_block).transpose(1, 0, 2), w_down.reshape(N_TP, hidden_block, D))
    results = lax.map(one_expert, (table, gate_weight, up_weight, down_weight))
    flat_index = ((ids * N_EP + source) * CAP + slot).reshape(-1)
    picked = results.reshape(EXPERTS * N_EP * CAP, D)[flat_index].reshape(TOKENS_B, TOP_K, D)
    expert_out = lax.optimization_barrier(jnp.sum(route_weight[..., None] * picked.astype(jnp.float32), axis=1)).astype(jnp.bfloat16)
    return (mixed, expert_out)
```

```python
import functools

import jax
import jax.numpy as jnp
import numpy as np
from jax import lax
from jax.experimental import pallas as pl
from jax.experimental.pallas import tpu as pltpu
from jax.sharding import PartitionSpec as P


F32 = jnp.float32
BF16 = jnp.bfloat16

GRID_W = 64


def rope_tables(count, offset, head_dim):
    pos = offset + lax.iota(jnp.int32, count)
    grid_row = (pos // GRID_W).astype(jnp.float32)
    grid_col = (pos % GRID_W).astype(jnp.float32)
    quarter = head_dim // 4
    inverse = 10000.0 ** (-jnp.arange(quarter, dtype=jnp.float32) / quarter)
    angles = jnp.concatenate([grid_row[:, None] * inverse, grid_col[:, None] * inverse], axis=-1)
    return (jnp.cos(angles), jnp.sin(angles))


def norm_rotate(x, gain, cosine, sine):
    count, number, head_dim = x.shape
    y = x * lax.rsqrt(jnp.mean(x * x, axis=-1, keepdims=True) + 1e-06) * gain
    pairs = y.reshape(count, number, head_dim // 2, 2)
    first, second = (pairs[..., 0], pairs[..., 1])
    cos_b = cosine[:, None, :]
    sin_b = sine[:, None, :]
    turned = jnp.stack([first * cos_b - second * sin_b, first * sin_b + second * cos_b], axis=-1)
    return turned.reshape(count, number, head_dim).astype(jnp.bfloat16)


def key_block_size(length, shard_rows):
    if length <= 2048:
        return length
    shards = length // shard_rows
    most = max(1, 2048 // shard_rows)
    best = 1
    for count in range(1, most + 1):
        if shards % count == 0:
            best = count
    return best * shard_rows


def plain_local(
    queries,
    keys,
    values,
    query_gain,
    key_gain,
    out_weight,
    expert_input,
    norm_gain,
    routes,
    route_logits,
    gate_weight,
    up_weight,
    down_weight,
):
    tokens_here = queries.shape[0]
    head_dim = query_gain.shape[0]
    heads_here = queries.shape[1] // head_dim
    kv_here = keys.shape[1] // head_dim
    group = heads_here // kv_here
    offset = lax.axis_index("ep") * tokens_here
    cosine, sine = rope_tables(tokens_here, offset, head_dim)
    q_rot = norm_rotate(
        queries.astype(jnp.float32).reshape(tokens_here, heads_here, head_dim),
        query_gain,
        cosine,
        sine,
    )
    k_rot = norm_rotate(
        keys.astype(jnp.float32).reshape(tokens_here, kv_here, head_dim), key_gain, cosine, sine
    ).reshape(tokens_here, kv_here * head_dim)
    q_grouped = q_rot.reshape(tokens_here, kv_here, group, head_dim).transpose(1, 2, 0, 3)
    q_grouped = q_grouped.reshape(kv_here, group * tokens_here, head_dim)
    query_rows = group * tokens_here
    scale = head_dim ** (-0.5)
    start_state = (
        jnp.full((kv_here, query_rows), -1e30, jnp.float32),
        jnp.zeros((kv_here, query_rows), jnp.float32),
        jnp.zeros((kv_here, query_rows, head_dim), jnp.float32),
    )
    key_piece = lax.all_gather(k_rot, "ep", axis=0, tiled=True)
    value_piece = lax.all_gather(values, "ep", axis=0, tiled=True)
    length = key_piece.shape[0]
    block = key_block_size(length, tokens_here)
    key_blocks = key_piece.reshape(length // block, block, kv_here, head_dim)
    value_blocks = value_piece.reshape(length // block, block, kv_here, head_dim)

    def step(state, blocks):
        running_max, running_total, running_sum = state
        key_block, value_block = blocks
        scores = (
            jnp.einsum("kqd,lkd->kql", q_grouped, key_block, preferred_element_type=jnp.float32)
            * scale
        )
        new_max = jnp.maximum(running_max, jnp.max(scores, axis=-1))
        factor = jnp.exp(running_max - new_max)
        weights = jnp.exp(scores - new_max[..., None])
        new_total = running_total * factor + jnp.sum(weights, axis=-1)
        new_sum = running_sum * factor[..., None] + jnp.einsum(
            "kql,lkd->kqd",
            weights.astype(jnp.bfloat16),
            value_block,
            preferred_element_type=jnp.float32,
        )
        return ((new_max, new_total, new_sum), None)

    result, _ = lax.scan(step, start_state, (key_blocks, value_blocks))
    _, final_total, final_sum = result
    attended = (final_sum / final_total[..., None]).astype(jnp.bfloat16)
    attended = attended.reshape(kv_here, group, tokens_here, head_dim).transpose(2, 0, 1, 3)
    attended = attended.reshape(tokens_here, heads_here * head_dim)
    summed = lax.psum_scatter(
        jnp.dot(attended, out_weight, preferred_element_type=jnp.float32).astype(jnp.bfloat16),
        "tp",
        scatter_dimension=0,
        tiled=True,
    ).astype(jnp.float32)
    mixed = summed.astype(jnp.bfloat16)
    expert_tokens_here, width = expert_input.shape
    n_ep = lax.axis_size("ep")
    top = routes.shape[1]
    capacity = expert_tokens_here * top // n_ep * 5 // 4
    x = expert_input.astype(jnp.float32)
    normed = (x * lax.rsqrt(jnp.mean(x * x, axis=-1, keepdims=True) + 1e-06) * norm_gain).astype(
        jnp.bfloat16
    )
    expert_ids = routes.reshape(-1)
    onehot = (expert_ids[:, None] == lax.iota(jnp.int32, n_ep)[None, :]).astype(jnp.int32)
    before = jnp.cumsum(onehot, axis=0) - onehot
    slot = jnp.sum(before * onehot, axis=1)
    target = expert_ids * capacity + slot
    owner_row = lax.iota(jnp.int32, expert_tokens_here * top) // top
    w_gate = gate_weight[0]
    w_up = up_weight[0]
    w_down = down_weight[0]
    columns = normed.shape[1]
    filled = jnp.zeros((n_ep * capacity, columns), jnp.bfloat16).at[target].set(normed[owner_row])
    arrived = lax.all_to_all(
        filled.reshape(n_ep, capacity, columns), "ep", split_axis=0, concat_axis=0, tiled=True
    )
    sources, slots, work_columns = arrived.shape
    flat = arrived.reshape(sources * slots, work_columns)
    gate = jnp.dot(flat, w_gate, preferred_element_type=jnp.float32)
    upper = jnp.dot(flat, w_up, preferred_element_type=jnp.float32)
    hidden = (jax.nn.silu(gate) * upper).astype(jnp.bfloat16)
    partial_out = jnp.dot(hidden, w_down, preferred_element_type=jnp.float32)
    summed = lax.psum_scatter(
        partial_out.reshape(sources, slots, width).astype(jnp.bfloat16),
        "tp",
        scatter_dimension=2,
        tiled=True,
    ).astype(jnp.float32)
    returned = lax.all_to_all(
        summed.astype(jnp.bfloat16), "ep", split_axis=0, concat_axis=0, tiled=True
    )
    picked = returned.reshape(n_ep * capacity, -1)[target].reshape(expert_tokens_here, top, -1)
    route_weight = jax.nn.sigmoid(route_logits - route_logits[:, ::-1])
    combined = jnp.sum(route_weight[..., None] * picked.astype(jnp.float32), axis=1)
    expert_out = combined.astype(jnp.bfloat16)
    return (mixed, expert_out)


def swap(x, axis, mask):
    return lax.ppermute(x, axis, [(i, i ^ mask) for i in range(lax.axis_size(axis))])


def spread_out(xs, axis, stride):
    return [x if not i else swap(x, axis, stride * i) for i, x in enumerate(xs)]


def call(body, outs, flops, moved, scratch=(), raw=0, shapes=(), kept=0):
    vmem = pl.BlockSpec(memory_space=pltpu.VMEM)
    hbm = pl.BlockSpec(memory_space=pl.ANY)
    scratch = list(scratch) + [pltpu.VMEM(x.shape, x.dtype) for x in shapes]
    if raw:
        scratch.append(pltpu.SemaphoreType.DMA((raw,)))

    def run(*args):
        args = [pltpu.with_memory_space_constraint(x, pltpu.HBM) for x in args[:raw]] + list(args[raw:])
        return pl.pallas_call(
            body,
            out_shape=[pltpu.VMEM(s, d) for s, d in outs[:kept]]
            + [jax.ShapeDtypeStruct(s, d) for s, d in outs[kept:]],
            in_specs=[hbm] * raw + [vmem] * (len(args) - raw),
            out_specs=[vmem for _ in outs],
            scratch_shapes=scratch,
            compiler_params=pltpu.CompilerParams(vmem_limit_bytes=16 << 20),
            cost_estimate=pl.CostEstimate(flops=flops, transcendentals=0, bytes_accessed=moved),
        )(*args)

    return run


def fetch(sources, targets, sems):
    copies = [
        pltpu.make_async_copy(a, b, sems.at[i]) for i, (a, b) in enumerate(zip(sources, targets))
    ]
    for copy in copies:
        copy.start()
    return copies


def wide(ref, offset, size):
    return ref[:, pl.ds(pl.multiple_of(offset, 128), size)]


def rope_body(*refs, head_dim, group, heads):
    (q_hbm, k_hbm, v_hbm, qg_hbm, kg_hbm, inv_hbm), weights = refs[:6], refs[6:9]
    stored, outs, loaded, sems = refs[9:12], refs[12:-7], refs[-7:-1], refs[-1]
    copies = fetch(refs[:6] + weights, loaded + stored, sems)
    q_ref, k_ref, v_ref, qg_ref, kg_ref, inv_ref = loaded
    count = q_ref.shape[0]
    me = lax.axis_index("ep")
    side = (me // 2) & 1
    lane = lax.broadcasted_iota(jnp.int32, (count, head_dim), 1)
    pos = me * count + lax.broadcasted_iota(jnp.int32, (count, head_dim), 0)
    shift = GRID_W.bit_length() - 1
    spot = jnp.where(lane < head_dim // 2, pos >> shift, pos & (GRID_W - 1)).astype(F32)
    for copy in copies[:6]:
        copy.wait()
    angle = spot * inv_ref[...]
    even = (lane & 1) == 0
    cosine = jnp.cos(angle)
    sine = jnp.sin(angle)
    sine = jnp.where(even, -sine, sine)

    def turn(x, gain):
        x = x.astype(F32)
        y = x * lax.rsqrt(jnp.mean(x * x, axis=-1, keepdims=True) + 1e-06) * gain
        other = jnp.where(even, pltpu.roll(y, head_dim - 1, 1), pltpu.roll(y, 1, 1))
        return (y * cosine + other * sine).astype(BF16)

    q_gain, k_gain = qg_ref[...], kg_ref[...]
    q0, kv0, pair, kv1 = outs
    for turned_side, q_outs, kv_outs in (
        (side, [(q0, 0)], [(kv0, 0)]),
        (side ^ 1, [(pair, 0)], [(pair, count), (kv1, 0)]),
    ):
        for h in range(heads * group):
            x = turn(wide(q_ref, (turned_side * heads * group + h) * head_dim, head_dim), q_gain)
            for out, row in q_outs:
                out[row : row + count, h * head_dim : (h + 1) * head_dim] = x
        for h in range(heads):
            at = (turned_side * heads + h) * head_dim
            x, v = turn(wide(k_ref, at, head_dim), k_gain), wide(v_ref, at, head_dim)
            for out, row in kv_outs:
                out[row : row + count, h * head_dim : (h + 1) * head_dim] = x
                out[row : row + count, (heads + h) * head_dim : (heads + h + 1) * head_dim] = v
    for copy in copies[6:]:
        copy.wait()


def attend_body(q0, q1, own, other, out0, out1, all_kv, *, head_dim, group, heads):
    count = q0.shape[0]
    half = own.shape[0]
    all_kv[:half, :] = own[...]
    all_kv[half:, :] = other[...]
    factor = float(head_dim) ** -0.5 * float(np.log2(np.e))
    for j in range(heads):
        keys = all_kv[:, j * head_dim : (j + 1) * head_dim]
        values = all_kv[:, (heads + j) * head_dim : (heads + j + 1) * head_dim]
        for q_ref, out in ((q0, out0), (q1, out1)):
            cols = [
                slice(h * head_dim, (h + 1) * head_dim)
                for h in range(j * group, (j + 1) * group)
            ]
            q = jnp.concatenate([q_ref[:, c] for c in cols], axis=0)
            s = lax.dot_general(q, keys, (((1,), (1,)), ((), ())), preferred_element_type=F32)
            top = jnp.max(s, axis=-1, keepdims=True)
            p = jnp.exp2((s - top) * factor)
            total = jnp.sum(p, axis=-1, keepdims=True)
            o = jnp.dot(p.astype(BF16), values, preferred_element_type=F32)
            o = (o / total).astype(BF16)
            for i, c in enumerate(cols):
                out[:, c] = o[i * count : (i + 1) * count, :]


def project_body(*refs, splits):
    pieces, w_ref, outs, whole = refs[:2], refs[2], refs[3 : 3 + splits], refs[3 + splits]
    side = (lax.axis_index("ep") // 2) & 1
    here = lax.axis_index("tp")
    cols = pieces[0].shape[1]
    acc = None
    for k, piece in enumerate(pieces):
        at = pl.multiple_of((side ^ k) * cols, cols)
        part = jnp.dot(piece[...], w_ref[pl.ds(at, cols), :], preferred_element_type=F32)
        acc = part if acc is None else acc + part
    whole[...] = acc
    rows = outs[0].shape[0]
    for i, out in enumerate(outs):
        out[...] = whole[pl.ds(pl.multiple_of((here ^ i) * rows, rows), rows), :].astype(BF16)


def dispatch_body(x0_hbm, g_hbm, x1_ref, r0_ref, r1_ref, *refs, chips, capacity, experts):
    own, sends = refs[0], refs[1:chips]
    picks, (normed, x0_ref, g_ref, sems) = refs[chips : chips + 2], refs[chips + 2 :]
    copies = fetch((x0_hbm, g_hbm), (x0_ref, g_ref), sems)
    count, _ = x0_ref.shape
    me = lax.axis_index("ep")
    chip, core = me // 2, me & 1
    rows = chips * 2 * capacity

    def spread(shape, axis):
        return lax.broadcasted_iota(jnp.int32, shape, axis)

    ahead = (spread((count, count), 0) < spread((count, count), 1)).astype(BF16)
    row = spread((rows, count), 0)
    block = ((row.astype(F32) + 0.5) * (1.0 / capacity)).astype(jnp.int32)
    slot = (row - block * capacity).astype(F32)
    side = block & 1
    row_e = spread((rows, experts), 0)
    block_e = ((row_e.astype(F32) + 0.5) * (1.0 / capacity)).astype(jnp.int32)
    target = 2 * (chip ^ (block_e >> 1)) + core
    chooser = (target == spread((rows, experts), 1)).astype(BF16)
    for i, ref in enumerate((r0_ref, r1_ref)):
        named = [
            (ref[j : j + 1, :] == spread((experts, count), 0)).astype(BF16) for j in range(2)
        ]
        before = jnp.dot(named[0] + named[1], ahead, preferred_element_type=F32)
        at = jnp.dot(chooser, before.astype(BF16), preferred_element_type=F32)
        fits = (at == slot) & (side == i)
        for j in range(2):
            hit = jnp.dot(chooser, named[j], preferred_element_type=F32)
            picks[j][:, i * count : (i + 1) * count] = jnp.where(fits & (hit > 0.5), 1.0, 0.0).astype(
                BF16
            )
    for copy in copies:
        copy.wait()
    for i, ref in enumerate((x0_ref, x1_ref)):
        x = ref[...].astype(F32)
        y = x * lax.rsqrt(jnp.mean(x * x, axis=-1, keepdims=True) + 1e-06) * g_ref[...]
        normed[i * count : (i + 1) * count, :] = y.astype(BF16)

    both = picks[0][...] + picks[1][...]
    step = 2 * capacity
    own[...] = jnp.dot(both[:step], normed[...], preferred_element_type=F32).astype(BF16)
    part = wide(normed, lax.axis_index("tp") * sends[0].shape[1], sends[0].shape[1])
    far = jnp.dot(both[step:], part, preferred_element_type=F32).astype(BF16)
    for k, out in enumerate(sends):
        out[...] = far[k * step : (k + 1) * step, :]


def expert_body(*refs, blocks):
    xs = refs[:blocks]
    wg, wu, wd = refs[blocks : blocks + 3]
    outs = refs[blocks + 3 :]
    here = lax.axis_index("tp")
    cols = xs[0].shape[1]
    across = (((1,), (1,)), ((), ()))
    gate = upper = None
    for i, x_ref in enumerate(xs):
        x = x_ref[...]
        at = (here ^ i) * cols if blocks > 1 else 0
        g = lax.dot_general(x, wide(wg, at, cols), across, preferred_element_type=F32)
        u = lax.dot_general(x, wide(wu, at, cols), across, preferred_element_type=F32)
        gate = g if gate is None else gate + g
        upper = u if upper is None else upper + u
    hidden = (jax.nn.silu(gate) * upper).astype(BF16)
    cols = outs[0].shape[1]
    for i, out in enumerate(outs):
        w = wide(wd, (here ^ i) * cols, cols)
        out[...] = jnp.dot(hidden, w, preferred_element_type=F32).astype(BF16)


def combine_body(l0_ref, l1_ref, p0_ref, p1_ref, *refs, chips, splits):
    homes, backs = refs[:splits], refs[splits : splits + chips - 1]
    mine, theirs, table = refs[splits + chips - 1 :]
    step, cols = homes[0].shape
    total = homes[0][...].astype(F32)
    for ref in homes[1:]:
        total = total + ref[...].astype(F32)
    table[:step, :] = total.astype(BF16)
    for k, ref in enumerate(backs):
        table[(k + 1) * step : (k + 2) * step, :] = ref[...]
    count = l0_ref.shape[1]
    flip = (((0,), (0,)), ((), ()))
    picked = [
        lax.dot_general(ref[...], table[...], flip, preferred_element_type=F32)
        for ref in (p0_ref, p1_ref)
    ]
    for i, (ref, out) in enumerate(((l0_ref, mine), (l1_ref, theirs))):
        gap = ref[0:1, :] - ref[1:2, :]
        first = jnp.broadcast_to(jax.nn.sigmoid(gap), (count, count)).T
        second = jnp.broadcast_to(jax.nn.sigmoid(-gap), (count, count)).T
        rows = slice(i * count, (i + 1) * count)
        for at in range(0, out.shape[1], count):
            cols = slice(at, at + count)
            out[:, cols] = first * picked[0][rows, cols] + second * picked[1][rows, cols]


def local(
    queries,
    keys,
    values,
    query_gain,
    key_gain,
    out_weight,
    expert_input,
    norm_gain,
    routes,
    route_logits,
    gate_weight,
    up_weight,
    down_weight,
):
    n_ep, n_tp = lax.axis_size("ep"), lax.axis_size("tp")
    chips = n_ep // 2
    count = queries.shape[0]
    head_dim = query_gain.shape[0]
    kv_here = keys.shape[1] // head_dim
    group = queries.shape[1] // keys.shape[1]
    tokens, width = expert_input.shape
    part = width // n_tp
    capacity = tokens * routes.shape[1] // n_ep * 5 // 4
    step = 2 * capacity
    rows = chips * step
    hidden = gate_weight.shape[2]

    routes, route_logits = routes.T, route_logits.T
    x_other = swap(expert_input, "ep", 1)
    routes_other = swap(routes, "ep", 1)
    logits_other = swap(route_logits, "ep", 1)
    sources = (expert_input, norm_gain.reshape(1, width))
    made = call(
        functools.partial(dispatch_body, chips=chips, capacity=capacity, experts=n_ep),
        [((step, width), BF16)]
        + [((step, part), BF16)] * (chips - 1)
        + [((rows, 2 * tokens), BF16)] * 2,
        2 * rows * 2 * tokens * width,
        4 * tokens * width,
        [pltpu.VMEM((2 * tokens, width), BF16)],
        raw=2,
        shapes=sources,
    )(*sources, x_other, routes, routes_other)
    own, picks = made[0], made[chips:]
    arrived = spread_out(made[:chips], "ep", 2)[1:]
    far = jnp.concatenate(arrived, axis=0)

    quarter = head_dim // 4
    inverse = (10000.0 ** (-np.arange(quarter, dtype=np.float32) / quarter)).astype(np.float32)
    inverse = np.tile(np.repeat(inverse, 2), 2).reshape(1, head_dim)
    heads = kv_here // 2
    q_cols, kv_cols = heads * group * head_dim, 2 * heads * head_dim
    gains = (query_gain.reshape(1, head_dim), key_gain.reshape(1, head_dim))
    sources = (queries, keys, values, *gains, jnp.asarray(inverse))
    weights = (gate_weight[0].T, up_weight[0].T, down_weight[0])
    made = call(
        functools.partial(rope_body, head_dim=head_dim, group=group, heads=heads),
        [(w.shape, BF16) for w in weights]
        + [((count, q_cols), BF16), ((count, kv_cols), BF16)]
        + [((2 * count, kv_cols), BF16), ((count, kv_cols), BF16)],
        count * queries.shape[1] * 60,
        4 * count * queries.shape[1] + 6 * width * hidden,
        raw=9,
        shapes=sources,
        kept=3,
    )(*sources, *weights)
    weights, (q0, kv0, pair, kv1) = made[:3], made[3:]
    pair = swap(pair, "ep", 2)
    blocks = [kv0, pair[count:]]
    blocks += [swap((kv0, kv1)[k & 1], "ep", 2 * k) for k in range(2, chips)]

    def expert(xs):
        number = xs[0].shape[0]
        return call(
            functools.partial(expert_body, blocks=len(xs)),
            [((number, part), BF16)] * n_tp,
            6 * number * width * hidden,
            6 * width * hidden,
        )(*xs, *weights)

    def add_up(xs):
        total = xs[0].astype(F32)
        for x in xs[1:]:
            total = total + x.astype(F32)
        return total.astype(BF16)

    home = spread_out(expert([own]), "tp", 1)
    gathered = spread_out([far] * n_tp, "tp", 1)

    kv_own = jnp.concatenate(blocks, axis=0)
    out0, out1 = call(
        functools.partial(attend_body, head_dim=head_dim, group=group, heads=heads),
        [((count, q_cols), BF16)] * 2,
        8 * count * q_cols * n_ep * count,
        8 * n_ep * count * kv_cols,
        [pltpu.VMEM((n_ep * count, kv_cols), BF16)],
    )(q0, pair[:count], kv_own, swap(kv_own, "ep", 1))
    attended = (out0, swap(out1, "ep", 2))

    remote = add_up(spread_out(expert(gathered), "tp", 1))
    backs = [remote] + [remote[k * step : (k + 1) * step] for k in range(chips - 1)]
    backs = spread_out(backs, "ep", 2)[1:]

    mixed = call(
        functools.partial(project_body, splits=n_tp),
        [((count // n_tp, width), BF16)] * n_tp,
        2 * count * out_weight.shape[0] * width,
        2 * out_weight.shape[0] * width,
        [pltpu.VMEM((count, width), F32)],
    )(*attended, out_weight)
    mixed = add_up(spread_out(mixed, "tp", 1))

    mine, theirs = call(
        functools.partial(combine_body, chips=chips, splits=n_tp),
        [((tokens, part), F32)] * 2,
        4 * rows * 2 * tokens * part,
        4 * rows * part,
        [pltpu.VMEM((rows, part), BF16)],
    )(route_logits, logits_other, *picks, *home, *backs)
    expert_out = (mine + swap(theirs, "ep", 1)).astype(BF16)
    return (mixed, expert_out)


def power_of_two(x):
    return x & (x - 1) == 0


def suits(mesh, shapes):
    n_ep, n_tp = mesh.shape["ep"], mesh.shape["tp"]
    queries, keys, gain, x, routes = shapes
    if n_ep < 4 or not (power_of_two(n_ep) and power_of_two(n_tp)):
        return False
    count, head_dim = queries[0] // n_ep, gain[0]
    tokens = x[0] // n_ep
    capacity = tokens * routes[1] // n_ep * 5 // 4
    return (
        head_dim % 128 == 0
        and keys[1] // n_tp % (2 * head_dim) == 0
        and queries[1] == 2 * keys[1]
        and count % (16 * n_tp) == 0
        and tokens % 128 == 0
        and capacity % 8 == 0
        and x[1] % (128 * n_tp) == 0
        and routes[1] == 2
    )


def solution(mesh):
    placed = (
        P("ep", "tp"),
        P("ep", "tp"),
        P("ep", "tp"),
        P(),
        P(),
        P("tp", None),
        P("ep", None),
        P(),
        P("ep", None),
        P("ep", None),
        P("ep", None, "tp"),
        P("ep", None, "tp"),
        P("ep", "tp", None),
    )

    sharded = functools.partial(
        jax.shard_map,
        mesh=mesh,
        in_specs=placed,
        out_specs=(P(("ep", "tp"), None), P("ep", "tp")),
        check_vma=False,
    )

    def run(*args):
        shapes = [args[j].shape for j in (0, 1, 3, 6, 8)]
        if not suits(mesh, shapes):
            return sharded(plain_local)(*args)
        return sharded(local)(*args)

    return run
```
